32 devices in a mesh: sp: 8 (over z, y), tp: 4 (over x, core).
Axes of the slice: x: 2, y: 2, z: 4, core: 2. Of those that a mesh axis runs over, the one named last changes fastest.
Arguments:
- stream: bfloat16 [3072, 2048], P(('sp', 'tp')), may hold values from -6 to 6
- query_projected: bfloat16 [3072, 1024], P('sp', 'tp'), may hold values from -6 to 6
- key_projected: bfloat16 [3072, 1024], P('sp', 'tp'), may hold values from -6 to 6
- value_projected: bfloat16 [3072, 1024], P('sp', 'tp'), may hold values from -6 to 6
- gate_projected: bfloat16 [3072, 1024], P('sp', 'tp'), may hold values from -6 to 6
- strength_logits: bfloat16 [8, 3072], P('tp', 'sp'), may hold values from -7 to 4
- decay_preactivation: bfloat16 [8, 3072], P('tp', 'sp'), may hold values from -9 to 9
- extra_log_decay: float32 [8, 3072], P('tp', 'sp'), may hold values from -0.7 to 0
- head_decay_rate: float32 [8], P('tp'), may hold values from 0 to 0.1
- head_norm_gain: float32 [128], replicated, may hold values from 0.1 to 1.9
- head_output_matrix: bfloat16 [1024, 2048], P('tp'), may hold values from -0.1875 to 0.1875
- feed_norm_gain: float32 [2048], replicated, may hold values from 0.1 to 1.9
- gate_matrix: bfloat16 [2048, 5632], P('sp', 'tp'), may hold values from -0.125 to 0.125
- up_matrix: bfloat16 [2048, 5632], P('sp', 'tp'), may hold values from -0.125 to 0.125
- down_matrix: bfloat16 [5632, 2048], P('tp', 'sp'), may hold values from -0.078125 to 0.078125
Outputs:
- result: bfloat16 [3072, 2048], P(('sp', 'tp'))
The draws below stay inside these ranges and needn't reach their ends.
All inputs are finite; a program needn't handle non-finite values.
Results may differ from the reference program's by a relative error of at most 0.015.
Values may be sent and summed in bfloat16 or wider, within the bound.
No kernel may reach another device: no remote copies, remote signals or barrier semaphores. Data moves between devices by JAX's collectives and lax.ppermute only.
A program may use at most 128 MiB of HBM per device.

```python
import math
import jax
import jax.numpy as jnp
from jax import lax

D = 2048
HEADS = 8
HEAD = 128
FF = 5632
BLOCK = 64
TOK_DEV = 384
HK = 1024
TOKENS = 3072
N_TP = 4


def head_ranking(key):
    return jax.random.permutation(jax.random.fold_in(key, 101), HEADS)


def fast_heads(key):
    fast_count = HEADS // 2
    return head_ranking(key) < fast_count


def draw_head_decay_rate(key, part):
    is_fast = fast_heads(key)
    slow_rate = jnp.exp(jax.random.uniform(jax.random.fold_in(key, 102), (HEADS,), jnp.float32, math.log(0.01), math.log(0.3))) / TOKENS
    fast_rate = jnp.exp(jax.random.uniform(jax.random.fold_in(key, 103), (HEADS,), jnp.float32, math.log(0.03), math.log(0.1)))
    return jnp.where(is_fast, fast_rate, slow_rate).astype(jnp.float32)


def draw_strength_logits(key, part):
    is_fast = fast_heads(key)
    fast_part = jnp.clip(jax.random.normal(jax.random.fold_in(key, 401), (HEADS, TOKENS), jnp.float32), -4.0, 4.0)
    faint_part = jax.random.uniform(jax.random.fold_in(key, 402), (HEADS, TOKENS), jnp.float32, -7.0, -5.0)
    return jnp.where(is_fast[:, None], fast_part, faint_part).astype(jnp.bfloat16)


def draw_decay_preactivation(key, part):
    block_total = TOKENS // TOK_DEV
    noise = jnp.clip(jax.random.normal(jax.random.fold_in(key, 201), (HEADS, block_total, TOK_DEV), jnp.float32), -6.0, 6.0)
    offsets = jax.random.uniform(jax.random.fold_in(key, 202), (block_total,), jnp.float32, -1.5, 1.5)
    return (noise + offsets[None, :, None]).reshape(HEADS, TOKENS).astype(jnp.bfloat16)


def draw_extra_log_decay(key, part):
    places = jax.random.randint(jax.random.fold_in(key, 301), (3,), 0, TOKENS)
    levels = jax.random.uniform(jax.random.fold_in(key, 302), (HEADS, 3), jnp.float32, math.log(0.5), math.log(0.8))
    base = jnp.zeros((HEADS, TOKENS), jnp.float32)
    return base.at[:, places].set(levels).astype(jnp.float32)


def steps_of(stream_key, extent, pieces, low, largest):
    def one(dim, blocks):
        heights = jax.random.uniform(jax.random.fold_in(jax.random.fold_in(stream_key, 6), dim), (blocks,), jnp.float32, low / len(pieces), largest / len(pieces))
        return jnp.repeat(jnp.exp(heights), extent[dim] // blocks).reshape((-1,) + (1,) * (len(extent) - dim - 1))

    level = one(*pieces[0])
    for cut in pieces[1:]:
        level = level * one(*cut)
    return level


def bell_draw(own_key, extent, scale, reach, cuts=(), kind=jnp.bfloat16):
    loudness = steps_of(own_key, extent, cuts, -0.22, 0.18) if cuts else 1.0
    values = jax.random.normal(own_key, extent, jnp.float32) * scale * loudness
    return jnp.minimum(jnp.maximum(values, -reach), reach).astype(kind)


def setup_inputs(seed: int = 0) -> dict:
    seeds = jax.random.split(jax.random.key(seed), 16)
    stream = bell_draw(seeds[0], (TOKENS, D), 1.0, 6.0, ((0, 32),))
    query_projected = bell_draw(seeds[1], (TOKENS, HK), 1.0, 6.0, ((0, 8), (1, 4)))
    key_projected = bell_draw(seeds[2], (TOKENS, HK), 1.0, 6.0, ((0, 8), (1, 4)))
    value_projected = bell_draw(seeds[3], (TOKENS, HK), 1.0, 6.0, ((0, 8), (1, 4)))
    gate_projected = bell_draw(seeds[4], (TOKENS, HK), 1.0, 6.0, ((0, 8), (1, 4)))
    strength_logits = draw_strength_logits(jax.random.fold_in(seeds[15], 71), 0)
    decay_preactivation = draw_decay_preactivation(jax.random.fold_in(seeds[15], 71), 0)
    extra_log_decay = draw_extra_log_decay(jax.random.fold_in(seeds[15], 71), 0)
    head_decay_rate = draw_head_decay_rate(jax.random.fold_in(seeds[15], 71), 0)
    head_norm_gain = jnp.clip(1.0 + 0.18 * jax.random.normal(seeds[9], (HEAD,), jnp.float32), 0.1, 1.9)
    head_output_matrix = bell_draw(seeds[10], (HK, D), HK ** -0.5, 0.1875, ((0, 4),))
    feed_norm_gain = jnp.clip(1.0 + 0.18 * jax.random.normal(seeds[11], (D,), jnp.float32), 0.1, 1.9)
    gate_matrix = bell_draw(seeds[12], (D, FF), D ** -0.5, 0.125, ((0, 8), (1, 4)))
    up_matrix = bell_draw(seeds[13], (D, FF), D ** -0.5, 0.125, ((0, 8), (1, 4)))
    down_matrix = bell_draw(seeds[14], (FF, D), FF ** -0.5, 0.078125, ((0, 4), (1, 8)))
    return dict(stream=stream, query_projected=query_projected, key_projected=key_projected, value_projected=value_projected, gate_projected=gate_projected, strength_logits=strength_logits, decay_preactivation=decay_preactivation, extra_log_decay=extra_log_decay, head_decay_rate=head_decay_rate, head_norm_gain=head_norm_gain, head_output_matrix=head_output_matrix, feed_norm_gain=feed_norm_gain, gate_matrix=gate_matrix, up_matrix=up_matrix, down_matrix=down_matrix)


PRECISION_FULL = lax.Precision.HIGHEST
EPSILON = 1e-06

def unit_rows(tensor):
    return tensor * lax.rsqrt(lax.optimization_barrier(jnp.sum(tensor * tensor, axis=-1, keepdims=True)) + EPSILON)

def block_correction(unit_queries, unit_keys, complete_values, strength_logits, decay_preactivation, extra_log_decay, head_decay_rate):
    head_count, length, head_width = unit_queries.shape
    block_count = length // BLOCK

    def to_blocks(tensor):
        return tensor.reshape((head_count, block_count, BLOCK) + tensor.shape[2:])
    beta_gate = jax.nn.sigmoid(strength_logits.astype(jnp.float32))
    decay_logarithm = -head_decay_rate[:, None] * jax.nn.softplus(decay_preactivation.astype(jnp.float32)) + extra_log_decay
    query_block = to_blocks(unit_queries)
    key_block = to_blocks(unit_keys)
    value_block = to_blocks(complete_values)
    beta_block = to_blocks(beta_gate)
    cumulative = jnp.cumsum(to_blocks(decay_logarithm), axis=-1)
    causal = jnp.tril(jnp.ones((BLOCK, BLOCK), bool))
    strict = jnp.tril(jnp.ones((BLOCK, BLOCK), bool), -1)
    spread = cumulative[..., :, None] - cumulative[..., None, :]
    damping = jnp.where(causal, jnp.exp(jnp.where(causal, spread, 0.0)), 0.0)
    key_beta = key_block * beta_block[..., None]
    lower_part = jnp.einsum('hnid,hnjd->hnij', key_beta, key_block, precision=PRECISION_FULL) * jnp.where(strict, damping, 0.0)
    system = lower_part + jnp.eye(BLOCK, dtype=jnp.float32)
    right_side = jnp.concatenate([value_block * beta_block[..., None], key_beta * jnp.exp(cumulative)[..., None]], axis=-1)
    solved = lax.linalg.triangular_solve(system, right_side, left_side=True, lower=True, unit_diagonal=True)
    target_values = solved[..., :head_width]
    householder_weights = solved[..., head_width:]
    inner_scores = jnp.einsum('hnid,hnjd->hnij', query_block, key_block, precision=PRECISION_FULL) * damping
    decayed_queries = query_block * jnp.exp(cumulative)[..., None]
    closing_log_decay = cumulative[..., -1:]
    decayed_keys = key_block * jnp.exp(closing_log_decay - cumulative)[..., None]
    return (decayed_queries, decayed_keys, target_values, householder_weights, inner_scores, closing_log_decay)

def advance(running_state, items):
    decayed_queries, decayed_keys, target_values, householder_weights, inner_scores, closing_log_decay = items
    new_state = target_values - jnp.einsum('fdc,fcj->fdj', householder_weights, running_state, precision=PRECISION_FULL)
    layer_output = jnp.einsum('fdc,fcj->fdj', decayed_queries, running_state, precision=PRECISION_FULL)
    layer_output = layer_output + jnp.einsum('hij,hjv->hiv', inner_scores, new_state, precision=PRECISION_FULL)
    running_state = jnp.exp(closing_log_decay)[:, :, None] * running_state + jnp.einsum('xwp,xws->xps', decayed_keys, new_state, precision=PRECISION_FULL)
    return (running_state, layer_output)

def split_heads(tensor):
    return tensor.reshape(TOKENS, HEADS, HEAD).transpose(1, 0, 2).astype(jnp.float32)

def rms_scale(tensor):
    return tensor * lax.rsqrt(lax.optimization_barrier(jnp.mean(tensor * tensor, axis=-1, keepdims=True)) + EPSILON)

def reference(stream, query_projected, key_projected, value_projected, gate_projected, strength_logits, decay_preactivation, extra_log_decay, head_decay_rate, head_norm_gain, head_output_matrix, feed_norm_gain, gate_matrix, up_matrix, down_matrix):
    unit_queries = unit_rows(split_heads(query_projected)) * HEAD ** (-0.5)
    unit_keys = unit_rows(split_heads(key_projected))
    complete_values = split_heads(value_projected)
    score_terms = block_correction(unit_queries, unit_keys, complete_values, strength_logits, decay_preactivation, extra_log_decay, head_decay_rate)
    moved = tuple((jnp.moveaxis(tensor, 1, 0) for tensor in score_terms))
    initial = jnp.zeros((HEADS, HEAD, HEAD), jnp.float32)
    _, block_outputs = lax.scan(advance, initial, moved)
    attention_output = jnp.moveaxis(block_outputs, 0, 1).reshape(HEADS, TOKENS, HEAD)
    normed_heads = rms_scale(attention_output) * head_norm_gain
    gated = normed_heads.transpose(1, 0, 2).reshape(TOKENS, HK) * jax.nn.silu(gate_projected.astype(jnp.float32))
    mixed = gated.astype(jnp.bfloat16)
    group_width = HK // N_TP
    branch = jnp.zeros((TOKENS, D), jnp.float32)
    for group in range(N_TP):
        piece = jnp.dot(mixed[:, group * group_width:(group + 1) * group_width].astype(jnp.float32), head_output_matrix[group * group_width:(group + 1) * group_width].astype(jnp.float32), preferred_element_type=jnp.float32)
        branch = branch + piece.astype(jnp.bfloat16).astype(jnp.float32)
    residual = stream.astype(jnp.float32) + branch
    normed = (rms_scale(residual) * feed_norm_gain).astype(jnp.bfloat16)
    gate = jnp.dot(normed.astype(jnp.float32), gate_matrix.astype(jnp.float32), preferred_element_type=jnp.float32)
    up_value = jnp.dot(normed.astype(jnp.float32), up_matrix.astype(jnp.float32), preferred_element_type=jnp.float32)
    hidden = (jax.nn.silu(gate) * up_value).astype(jnp.bfloat16)
    unit_group = FF // N_TP
    ffn_total = jnp.zeros((TOKENS, D), jnp.float32)
    for group in range(N_TP):
        piece = jnp.dot(hidden[:, group * unit_group:(group + 1) * unit_group].astype(jnp.float32), down_matrix[group * unit_group:(group + 1) * unit_group].astype(jnp.float32), preferred_element_type=jnp.float32)
        ffn_total = ffn_total + piece.astype(jnp.bfloat16).astype(jnp.float32)
    return (residual + ffn_total).astype(jnp.bfloat16)
```

```python
import jax
import jax.numpy as jnp
from jax import lax
from jax.sharding import PartitionSpec as P

HEAD = 128
BLOCK = 64


PRECISION_FULL = lax.Precision.HIGHEST
EPSILON = 1e-06


def from_behind(value, axis, by):
    size = lax.axis_size(axis)
    pairs = [(i, i + by) for i in range(size) if 0 <= i + by < size]
    return lax.ppermute(value, axis, pairs)


def unit_rows(tensor):
    return tensor * lax.rsqrt(jnp.sum(tensor * tensor, axis=-1, keepdims=True) + EPSILON)


def rms_scale(tensor):
    return tensor * lax.rsqrt(jnp.mean(tensor * tensor, axis=-1, keepdims=True) + EPSILON)


def unit_lower_inverse(strict_lower):
    size = strict_lower.shape[-1]
    row = jnp.arange(size)[:, None]
    column = jnp.arange(size)[None, :]

    def corner(half):
        same_pair = row // (2 * half) == column // (2 * half)
        return jnp.where(same_pair & (row // half != column // half), strict_lower, 0.0)

    inverse = jnp.eye(size, dtype=jnp.float32) - corner(1)
    half = 2
    while half < size:
        left = jnp.einsum("hnij,hnjk->hnik", inverse, corner(half), precision=PRECISION_FULL)
        inverse = inverse - jnp.einsum(
            "hnij,hnjk->hnik", left, inverse, precision=PRECISION_FULL
        )
        half *= 2
    return inverse


def swap(value, axis, bit):
    size = lax.axis_size(axis)
    return lax.ppermute(value, axis, [(i, i ^ bit) for i in range(size)])


def relative_order(count):
    order = [0]
    bit = count // 2
    while bit:
        order = order + [place ^ bit for place in order]
        bit //= 2
    return order


def gather_relative(own):
    bit = lax.axis_size("tp") // 2
    while bit:
        own = jnp.concatenate([own, swap(own, "tp", bit)], axis=0)
        bit //= 2
    return own


def scatter_relative(left_rows, matrix):
    size = lax.axis_size("tp")
    if size == 1:
        return jnp.dot(left_rows, matrix, preferred_element_type=jnp.float32)
    half = left_rows.shape[0] // 2
    leaving = jnp.dot(left_rows[half:], matrix, preferred_element_type=jnp.float32)
    arrived = swap(leaving.astype(jnp.bfloat16), "tp", 1)
    total = jnp.dot(left_rows[:half], matrix, preferred_element_type=jnp.float32)
    total = total + arrived.astype(jnp.float32)
    bit = 2
    while bit < size:
        half = total.shape[0] // 2
        arrived = swap(total[half:].astype(jnp.bfloat16), "tp", bit)
        total = total[:half] + arrived.astype(jnp.float32)
        bit *= 2
    return total


def inflow_of_earlier(matrix_product, running_state):
    size = lax.axis_size("sp")
    width = running_state.shape[-1]
    pair = jnp.concatenate([matrix_product, running_state], axis=-1)
    pair = from_behind(pair.astype(jnp.bfloat16), "sp", 1).astype(jnp.float32)
    by = 1
    while by < size - 1:
        matrix, state = pair[..., :width], pair[..., width:]
        last = 2 * by >= size - 1
        sent = (state if last else pair).astype(jnp.bfloat16)
        earlier = from_behind(sent, "sp", by).astype(jnp.float32)
        moved = jnp.einsum("hij,hjk->hik", matrix, earlier, precision=PRECISION_FULL)
        if last:
            pair = jnp.concatenate([matrix, state + moved], axis=-1)
        else:
            pair = jnp.concatenate([moved[..., :width], state + moved[..., width:]], axis=-1)
        by *= 2
    return pair[..., width:]


def block_correction(
    unit_queries,
    unit_keys,
    complete_values,
    strength_logits,
    decay_preactivation,
    extra_log_decay,
    head_decay_rate,
):
    head_count, length, head_width = unit_queries.shape
    block_count = length // BLOCK

    def to_blocks(tensor):
        return tensor.reshape((head_count, block_count, BLOCK) + tensor.shape[2:])

    beta_gate = jax.nn.sigmoid(strength_logits.astype(jnp.float32))
    decay_logarithm = (
        -head_decay_rate[:, None] * jax.nn.softplus(decay_preactivation.astype(jnp.float32))
        + extra_log_decay
    )
    query_block = to_blocks(unit_queries)
    key_block = to_blocks(unit_keys)
    value_block = to_blocks(complete_values)
    beta_block = to_blocks(beta_gate)
    cumulative = jnp.cumsum(to_blocks(decay_logarithm), axis=-1)
    causal = jnp.tril(jnp.ones((BLOCK, BLOCK), bool))
    strict = jnp.tril(jnp.ones((BLOCK, BLOCK), bool), -1)
    spread = cumulative[..., :, None] - cumulative[..., None, :]
    damping = jnp.where(causal, jnp.exp(jnp.where(causal, spread, 0.0)), 0.0)
    key_beta = key_block * beta_block[..., None]
    lower_part = jnp.einsum(
        "hnid,hnjd->hnij", key_beta, key_block, precision=PRECISION_FULL
    ) * jnp.where(strict, damping, 0.0)
    right_side = jnp.concatenate(
        [value_block * beta_block[..., None], key_beta * jnp.exp(cumulative)[..., None]], axis=-1
    )
    solved = jnp.einsum(
        "hnij,hnjd->hnid", unit_lower_inverse(lower_part), right_side, precision=PRECISION_FULL
    )
    target_values = solved[..., :head_width]
    householder_weights = solved[..., head_width:]
    inner_scores = (
        jnp.einsum("hnid,hnjd->hnij", query_block, key_block, precision=PRECISION_FULL) * damping
    )
    decayed_queries = query_block * jnp.exp(cumulative)[..., None]
    closing_log_decay = cumulative[..., -1:]
    decayed_keys = key_block * jnp.exp(closing_log_decay - cumulative)[..., None]
    return (
        decayed_queries,
        decayed_keys,
        target_values,
        householder_weights,
        inner_scores,
        closing_log_decay,
    )


def local_recurrence(
    query_projected,
    key_projected,
    value_projected,
    strength_logits,
    decay_preactivation,
    extra_log_decay,
    head_decay_rate,
):
    head_count = strength_logits.shape[0]
    tok_count = strength_logits.shape[1]

    def split_heads(tensor):
        return tensor.reshape(tok_count, head_count, HEAD).transpose(1, 0, 2).astype(jnp.float32)

    unit_queries = unit_rows(split_heads(query_projected)) * HEAD ** (-0.5)
    unit_keys = unit_rows(split_heads(key_projected))
    complete_values = split_heads(value_projected)
    score_terms = block_correction(
        unit_queries,
        unit_keys,
        complete_values,
        strength_logits,
        decay_preactivation,
        extra_log_decay,
        head_decay_rate,
    )
    identity = jnp.broadcast_to(jnp.eye(HEAD, dtype=jnp.float32), (head_count, HEAD, HEAD))

    def advance(carry, items):
        running_state, matrix_product = carry
        (
            decayed_queries,
            decayed_keys,
            target_values,
            householder_weights,
            inner_scores,
            closing_log_decay,
        ) = items
        new_state = target_values - jnp.einsum(
            "fdc,fcj->fdj", householder_weights, running_state, precision=PRECISION_FULL
        )
        layer_output = jnp.einsum(
            "fdc,fcj->fdj", decayed_queries, running_state, precision=PRECISION_FULL
        )
        layer_output = layer_output + jnp.einsum(
            "hij,hjv->hiv", inner_scores, new_state, precision=PRECISION_FULL
        )
        passed_state = decayed_queries - jnp.einsum(
            "hij,hjk->hik", inner_scores, householder_weights, precision=PRECISION_FULL
        )
        decay_span = jnp.einsum(
            "fdc,fcj->fdj", passed_state, matrix_product, precision=PRECISION_FULL
        )
        decay_factor = jnp.exp(closing_log_decay)[:, :, None]
        step_map = decay_factor * identity - jnp.einsum(
            "hik,hij->hkj", decayed_keys, householder_weights, precision=PRECISION_FULL
        )
        running_state = decay_factor * running_state + jnp.einsum(
            "xwp,xws->xps", decayed_keys, new_state, precision=PRECISION_FULL
        )
        matrix_product = jnp.einsum(
            "hij,hjk->hik", step_map, matrix_product, precision=PRECISION_FULL
        )
        return ((running_state, matrix_product), (layer_output, decay_span))

    moved = tuple((jnp.moveaxis(tensor, 1, 0) for tensor in score_terms))
    zeros_state = jnp.zeros((head_count, HEAD, HEAD), jnp.float32)
    (running_state, matrix_product), (block_outputs, decay_spans) = lax.scan(
        advance, (zeros_state, identity), moved
    )

    def merge_blocks(tensor):
        return jnp.moveaxis(tensor, 0, 1).reshape(head_count, tok_count, HEAD)

    return (
        merge_blocks(block_outputs),
        merge_blocks(decay_spans),
        matrix_product,
        running_state,
        identity,
    )


def body(
    stream,
    query_projected,
    key_projected,
    value_projected,
    gate_projected,
    strength_logits,
    decay_preactivation,
    extra_log_decay,
    head_decay_rate,
    head_norm_gain,
    head_output_matrix,
    feed_norm_gain,
    gate_matrix,
    up_matrix,
    down_matrix,
):
    gate_whole = lax.all_gather(gate_matrix, "sp", axis=0, tiled=True)
    up_whole = lax.all_gather(up_matrix, "sp", axis=0, tiled=True)
    down_whole = lax.all_gather(down_matrix, "sp", axis=1, tiled=True)
    block_outputs, decay_spans, matrix_product, running_state, _ = local_recurrence(
        query_projected,
        key_projected,
        value_projected,
        strength_logits,
        decay_preactivation,
        extra_log_decay,
        head_decay_rate,
    )
    state_inflow = inflow_of_earlier(matrix_product, running_state)
    attention_output = block_outputs + jnp.einsum(
        "qwc,qcn->qwn", decay_spans, state_inflow, precision=PRECISION_FULL
    )
    head_count = attention_output.shape[0]
    tok_count = attention_output.shape[1]
    normed_heads = rms_scale(attention_output) * head_norm_gain
    gated = normed_heads.transpose(1, 0, 2).reshape(tok_count, head_count * HEAD)
    mixed = (gated * jax.nn.silu(gate_projected.astype(jnp.float32))).astype(jnp.bfloat16)
    tp_size = lax.axis_size("tp")
    tp_index = lax.axis_index("tp")
    chunks = mixed.reshape(tp_size, tok_count // tp_size, head_count * HEAD)
    ordered = jnp.concatenate(
        [
            lax.dynamic_index_in_dim(chunks, tp_index ^ place, 0, keepdims=False)
            for place in relative_order(tp_size)
        ],
        axis=0,
    )
    branch = scatter_relative(ordered, head_output_matrix)
    residual_own = stream.astype(jnp.float32) + branch
    normed_own = (rms_scale(residual_own) * feed_norm_gain).astype(jnp.bfloat16)
    whole_rows = gather_relative(normed_own)
    gate_total = jnp.dot(whole_rows, gate_whole, preferred_element_type=jnp.float32)
    up_total = jnp.dot(whole_rows, up_whole, preferred_element_type=jnp.float32)
    hidden = (jax.nn.silu(gate_total) * up_total).astype(jnp.bfloat16)
    ffn_own = scatter_relative(hidden, down_whole)
    return (residual_own + ffn_own).astype(jnp.bfloat16)


def solution(mesh):
    placed = (
        P(("sp", "tp"), None),
        P("sp", "tp"),
        P("sp", "tp"),
        P("sp", "tp"),
        P("sp", "tp"),
        P("tp", "sp"),
        P("tp", "sp"),
        P("tp", "sp"),
        P("tp"),
        P(),
        P("tp", None),
        P(),
        P("sp", "tp"),
        P("sp", "tp"),
        P("tp", "sp"),
    )
    return jax.shard_map(
        body, mesh=mesh, in_specs=placed, out_specs=P(("sp", "tp"), None), check_vma=False
    )
```

```python
import jax
import jax.numpy as jnp
from jax import lax
from jax.sharding import PartitionSpec as P

HEAD = 128
BLOCK = 64


PRECISION_FULL = lax.Precision.HIGHEST
EPSILON = 1e-06


def from_behind(value, axis, by):
    size = lax.axis_size(axis)
    pairs = [(i, i + by) for i in range(size) if 0 <= i + by < size]
    return lax.ppermute(value, axis, pairs)


def unit_rows(tensor):
    return tensor * lax.rsqrt(jnp.sum(tensor * tensor, axis=-1, keepdims=True) + EPSILON)


def rms_scale(tensor):
    return tensor * lax.rsqrt(jnp.mean(tensor * tensor, axis=-1, keepdims=True) + EPSILON)


def unit_lower_inverse(strict_lower):
    size = strict_lower.shape[-1]
    row = jnp.arange(size)[:, None]
    column = jnp.arange(size)[None, :]

    def corner(half):
        same_pair = row // (2 * half) == column // (2 * half)
        return jnp.where(same_pair & (row // half != column // half), strict_lower, 0.0)

    inverse = jnp.eye(size, dtype=jnp.float32) - corner(1)
    half = 2
    while half < size:
        left = jnp.einsum("hnij,hnjk->hnik", inverse, corner(half), precision=PRECISION_FULL)
        inverse = inverse - jnp.einsum(
            "hnij,hnjk->hnik", left, inverse, precision=PRECISION_FULL
        )
        half *= 2
    return inverse


def swap(value, axis, bit):
    size = lax.axis_size(axis)
    return lax.ppermute(value, axis, [(i, i ^ bit) for i in range(size)])


def relative_order(count):
    order = [0]
    bit = count // 2
    while bit:
        order = order + [place ^ bit for place in order]
        bit //= 2
    return order


def gather_relative(own):
    bit = lax.axis_size("tp") // 2
    while bit:
        own = jnp.concatenate([own, swap(own, "tp", bit)], axis=0)
        bit //= 2
    return own


def takes_blocks(sp_size):
    return sp_size % 2 == 0 and 4 <= sp_size <= 16


def blocks_of_sp(shard, early_partner):
    size = lax.axis_size("sp")
    outer = size // 2

    def along(by):
        return lax.ppermute(shard, "sp", [(i, (i + 2 * by) % size) for i in range(size)])

    turns = sorted(range(1, outer), key=lambda by: min(by, outer - by))
    near = {0: shard} | {by: along(by) for by in turns}
    far = {0: early_partner} | {by: swap(near[by], "sp", 1) for by in turns}
    return [near[by] for by in range(outer)] + [far[by] for by in range(outer)]


def block_sources():
    size = lax.axis_size("sp")
    outer = size // 2
    me = lax.axis_index("sp")
    return [
        ((me // 2 + outer - by) % outer) * 2 + ((me % 2) ^ flip)
        for flip in range(2)
        for by in range(outer)
    ]


def absolute_columns(value):
    size = lax.axis_size("sp")
    outer = size // 2
    width = value.shape[1] // size
    me = lax.axis_index("sp")
    pieces = []
    for index in range(size):
        by = (me // 2 + outer - index // 2) % outer
        place = by + outer * ((me % 2) ^ (index % 2))
        pieces.append(lax.dynamic_slice_in_dim(value, place * width, width, axis=1))
    return jnp.concatenate(pieces, axis=1)


def scatter_relative(left_rows, matrices):
    def times(rows):
        return jnp.concatenate(
            [jnp.dot(rows, matrix, preferred_element_type=jnp.float32) for matrix in matrices],
            axis=1,
        )

    size = lax.axis_size("tp")
    if size == 1:
        return times(left_rows)
    half = left_rows.shape[0] // 2
    leaving = times(left_rows[half:])
    arrived = swap(leaving.astype(jnp.bfloat16), "tp", 1)
    total = times(left_rows[:half])
    total = total + arrived.astype(jnp.float32)
    bit = 2
    while bit < size:
        half = total.shape[0] // 2
        arrived = swap(total[half:].astype(jnp.bfloat16), "tp", bit)
        total = total[:half] + arrived.astype(jnp.float32)
        bit *= 2
    return total


def inflow_of_earlier(matrix_product, running_state):
    size = lax.axis_size("sp")
    width = running_state.shape[-1]
    pair = jnp.concatenate([matrix_product, running_state], axis=-1)
    pair = from_behind(pair.astype(jnp.bfloat16), "sp", 1).astype(jnp.float32)
    by = 1
    while by < size - 1:
        matrix, state = pair[..., :width], pair[..., width:]
        last = 2 * by >= size - 1
        sent = (state if last else pair).astype(jnp.bfloat16)
        earlier = from_behind(sent, "sp", by).astype(jnp.float32)
        moved = jnp.einsum("hij,hjk->hik", matrix, earlier, precision=PRECISION_FULL)
        if last:
            pair = jnp.concatenate([matrix, state + moved], axis=-1)
        else:
            pair = jnp.concatenate([moved[..., :width], state + moved[..., width:]], axis=-1)
        by *= 2
    return pair[..., width:]


def block_correction(
    unit_queries,
    unit_keys,
    complete_values,
    strength_logits,
    decay_preactivation,
    extra_log_decay,
    head_decay_rate,
):
    head_count, length, head_width = unit_queries.shape
    block_count = length // BLOCK

    def to_blocks(tensor):
        return tensor.reshape((head_count, block_count, BLOCK) + tensor.shape[2:])

    beta_gate = jax.nn.sigmoid(strength_logits.astype(jnp.float32))
    decay_logarithm = (
        -head_decay_rate[:, None] * jax.nn.softplus(decay_preactivation.astype(jnp.float32))
        + extra_log_decay
    )
    query_block = to_blocks(unit_queries)
    key_block = to_blocks(unit_keys)
    value_block = to_blocks(complete_values)
    beta_block = to_blocks(beta_gate)
    cumulative = jnp.cumsum(to_blocks(decay_logarithm), axis=-1)
    causal = jnp.tril(jnp.ones((BLOCK, BLOCK), bool))
    strict = jnp.tril(jnp.ones((BLOCK, BLOCK), bool), -1)
    spread = cumulative[..., :, None] - cumulative[..., None, :]
    damping = jnp.where(causal, jnp.exp(jnp.where(causal, spread, 0.0)), 0.0)
    key_beta = key_block * beta_block[..., None]
    lower_part = jnp.einsum(
        "hnid,hnjd->hnij", key_beta, key_block, precision=PRECISION_FULL
    ) * jnp.where(strict, damping, 0.0)
    right_side = jnp.concatenate(
        [value_block * beta_block[..., None], key_beta * jnp.exp(cumulative)[..., None]], axis=-1
    )
    solved = jnp.einsum(
        "hnij,hnjd->hnid", unit_lower_inverse(lower_part), right_side, precision=PRECISION_FULL
    )
    target_values = solved[..., :head_width]
    householder_weights = solved[..., head_width:]
    inner_scores = (
        jnp.einsum("hnid,hnjd->hnij", query_block, key_block, precision=PRECISION_FULL) * damping
    )
    decayed_queries = query_block * jnp.exp(cumulative)[..., None]
    closing_log_decay = cumulative[..., -1:]
    decayed_keys = key_block * jnp.exp(closing_log_decay - cumulative)[..., None]
    return (
        decayed_queries,
        decayed_keys,
        target_values,
        householder_weights,
        inner_scores,
        closing_log_decay,
    )


def local_recurrence(
    query_projected,
    key_projected,
    value_projected,
    strength_logits,
    decay_preactivation,
    extra_log_decay,
    head_decay_rate,
):
    head_count = strength_logits.shape[0]
    tok_count = strength_logits.shape[1]

    def split_heads(tensor):
        return tensor.reshape(tok_count, head_count, HEAD).transpose(1, 0, 2).astype(jnp.float32)

    unit_queries = unit_rows(split_heads(query_projected)) * HEAD ** (-0.5)
    unit_keys = unit_rows(split_heads(key_projected))
    complete_values = split_heads(value_projected)
    score_terms = block_correction(
        unit_queries,
        unit_keys,
        complete_values,
        strength_logits,
        decay_preactivation,
        extra_log_decay,
        head_decay_rate,
    )
    identity = jnp.broadcast_to(jnp.eye(HEAD, dtype=jnp.float32), (head_count, HEAD, HEAD))

    def advance(carry, items):
        running_state, matrix_product = carry
        (
            decayed_queries,
            decayed_keys,
            target_values,
            householder_weights,
            inner_scores,
            closing_log_decay,
        ) = items
        new_state = target_values - jnp.einsum(
            "fdc,fcj->fdj", householder_weights, running_state, precision=PRECISION_FULL
        )
        layer_output = jnp.einsum(
            "fdc,fcj->fdj", decayed_queries, running_state, precision=PRECISION_FULL
        )
        layer_output = layer_output + jnp.einsum(
            "hij,hjv->hiv", inner_scores, new_state, precision=PRECISION_FULL
        )
        passed_state = decayed_queries - jnp.einsum(
            "hij,hjk->hik", inner_scores, householder_weights, precision=PRECISION_FULL
        )
        decay_span = jnp.einsum(
            "fdc,fcj->fdj", passed_state, matrix_product, precision=PRECISION_FULL
        )
        decay_factor = jnp.exp(closing_log_decay)[:, :, None]
        step_map = decay_factor * identity - jnp.einsum(
            "hik,hij->hkj", decayed_keys, householder_weights, precision=PRECISION_FULL
        )
        running_state = decay_factor * running_state + jnp.einsum(
            "xwp,xws->xps", decayed_keys, new_state, precision=PRECISION_FULL
        )
        matrix_product = jnp.einsum(
            "hij,hjk->hik", step_map, matrix_product, precision=PRECISION_FULL
        )
        return ((running_state, matrix_product), (layer_output, decay_span))

    moved = tuple((jnp.moveaxis(tensor, 1, 0) for tensor in score_terms))
    zeros_state = jnp.zeros((head_count, HEAD, HEAD), jnp.float32)
    (running_state, matrix_product), (block_outputs, decay_spans) = lax.scan(
        advance, (zeros_state, identity), moved
    )

    def merge_blocks(tensor):
        return jnp.moveaxis(tensor, 0, 1).reshape(head_count, tok_count, HEAD)

    return (
        merge_blocks(block_outputs),
        merge_blocks(decay_spans),
        matrix_product,
        running_state,
        identity,
    )


def body(
    stream,
    query_projected,
    key_projected,
    value_projected,
    gate_projected,
    strength_logits,
    decay_preactivation,
    extra_log_decay,
    head_decay_rate,
    head_norm_gain,
    head_output_matrix,
    feed_norm_gain,
    gate_matrix,
    up_matrix,
    down_matrix,
):
    gate_whole = lax.all_gather(gate_matrix, "sp", axis=0, tiled=True)
    sp_size = lax.axis_size("sp")
    by_blocks = takes_blocks(sp_size)
    if by_blocks:
        up_partner = swap(up_matrix, "sp", 1)
        down_partner = swap(down_matrix, "sp", 1)
    else:
        up_whole = lax.all_gather(up_matrix, "sp", axis=0, tiled=True)
        down_whole = lax.all_gather(down_matrix, "sp", axis=1, tiled=True)
    block_outputs, decay_spans, matrix_product, running_state, _ = local_recurrence(
        query_projected,
        key_projected,
        value_projected,
        strength_logits,
        decay_preactivation,
        extra_log_decay,
        head_decay_rate,
    )
    state_inflow = inflow_of_earlier(matrix_product, running_state)
    if by_blocks:
        state_inflow, up_matrix, down_matrix = lax.optimization_barrier(
            (state_inflow, up_matrix, down_matrix)
        )
        up_blocks = blocks_of_sp(up_matrix, up_partner)
        down_blocks = blocks_of_sp(down_matrix, down_partner)
    attention_output = block_outputs + jnp.einsum(
        "qwc,qcn->qwn", decay_spans, state_inflow, precision=PRECISION_FULL
    )
    head_count = attention_output.shape[0]
    tok_count = attention_output.shape[1]
    normed_heads = rms_scale(attention_output) * head_norm_gain
    gated = normed_heads.transpose(1, 0, 2).reshape(tok_count, head_count * HEAD)
    mixed = (gated * jax.nn.silu(gate_projected.astype(jnp.float32))).astype(jnp.bfloat16)
    tp_size = lax.axis_size("tp")
    tp_index = lax.axis_index("tp")
    chunks = mixed.reshape(tp_size, tok_count // tp_size, head_count * HEAD)
    ordered = jnp.concatenate(
        [
            lax.dynamic_index_in_dim(chunks, tp_index ^ place, 0, keepdims=False)
            for place in relative_order(tp_size)
        ],
        axis=0,
    )
    branch = scatter_relative(ordered, [head_output_matrix])
    residual_own = stream.astype(jnp.float32) + branch
    normed_own = (rms_scale(residual_own) * feed_norm_gain).astype(jnp.bfloat16)
    whole_rows = gather_relative(normed_own)
    gate_total = jnp.dot(whole_rows, gate_whole, preferred_element_type=jnp.float32)
    if by_blocks:
        width = up_matrix.shape[0]
        columns = [
            lax.dynamic_slice_in_dim(whole_rows, source * width, width, axis=1)
            for source in block_sources()
        ]
        half = sp_size // 2
        up_total = sum(
            jnp.dot(
                jnp.concatenate(columns[part], axis=1),
                jnp.concatenate(up_blocks[part], axis=0),
                preferred_element_type=jnp.float32,
            )
            for part in (slice(None, half), slice(half, None))
        )
    else:
        up_total = jnp.dot(whole_rows, up_whole, preferred_element_type=jnp.float32)
    hidden = (jax.nn.silu(gate_total) * up_total).astype(jnp.bfloat16)
    if by_blocks:
        ffn_own = absolute_columns(scatter_relative(hidden, down_blocks))
    else:
        ffn_own = scatter_relative(hidden, [down_whole])
    return (residual_own + ffn_own).astype(jnp.bfloat16)


def solution(mesh):
    placed = (
        P(("sp", "tp"), None),
        P("sp", "tp"),
        P("sp", "tp"),
        P("sp", "tp"),
        P("sp", "tp"),
        P("tp", "sp"),
        P("tp", "sp"),
        P("tp", "sp"),
        P("tp"),
        P(),
        P("tp", None),
        P(),
        P("sp", "tp"),
        P("sp", "tp"),
        P("tp", "sp"),
    )

    return jax.shard_map(
        body, mesh=mesh, in_specs=placed, out_specs=P(("sp", "tp"), None), check_vma=False
    )
```
